32 devices in a mesh: rep: 2 (over y), fs: 4 (over z), tp: 4 (over x, core).
Axes of the slice: x: 2, y: 2, z: 4, core: 2. Of those that a mesh axis runs over, the one named last changes fastest.
Arguments:
- activations: bfloat16 [8, 256, 2048], P(('rep', 'fs'), None, 'tp'), may hold values from -15 to 15
- norm_gain: float32 [2048], replicated, may hold values from 0.1 to 1.9
- w_value: bfloat16 [2048, 2048], P('fs', 'tp'), may hold values from -0.125 to 0.125
- w_gate_conv: bfloat16 [2048, 2048], P('fs', 'tp'), may hold values from -0.125 to 0.125
- conv_weight: float32 [31, 2048], P(None, 'tp'), may hold values from -3 to 3
- chan_gain: float32 [2048], P('tp'), may hold values from 0.1 to 1.9
- w_conv_out: bfloat16 [2048, 2048], P('tp', 'fs'), may hold values from -0.125 to 0.125
- mix_gain: float32 [2048], replicated, may hold values from 0.1 to 1.9
- w_gate: bfloat16 [2048, 3072], P('fs', 'tp'), may hold values from -0.125 to 0.125
- w_up: bfloat16 [2048, 3072], P('fs', 'tp'), may hold values from -0.125 to 0.125
- w_down: bfloat16 [3072, 2048], P('tp', 'fs'), may hold values from -0.109375 to 0.109375
- final_gain: float32 [2048], P('tp'), may hold values from 0.1 to 1.9
Outputs:
- result: bfloat16 [8, 256, 2048], P(('rep', 'fs'), None, 'tp')
The draws below stay inside these ranges and needn't reach their ends.
All inputs are finite; a program needn't handle non-finite values.
Results may differ from the reference program's by a relative error of at most 0.013.
Values may be sent and summed in bfloat16 or wider, within the bound.
A program may use at most 64 MiB of HBM per device.

```python
import jax
import jax.numpy as jnp
from jax import lax

D = 2048
C = 2048
FF = 3072
K = 31
SEQ = 256
BATCH = 8
N_TP = 4


def draw_activations(key, part):
    column = jnp.arange(D, dtype=jnp.float32)
    scale = 0.3 * 10.0 ** (column / (D - 1))
    values = jax.random.normal(key, (BATCH, SEQ, D), jnp.float32) * scale
    return jnp.clip(values, -15.0, 15.0).astype(jnp.bfloat16)


def draw_conv_weight(key, part):
    channel = jnp.arange(C, dtype=jnp.float32)
    scale = 0.35 * 8.0 ** (channel / (C - 1)) / jnp.sqrt(jnp.float32(K))
    values = jnp.clip(jax.random.normal(key, (K, C), jnp.float32), -4.0, 4.0) * scale
    return jnp.clip(values, -3.0, 3.0).astype(jnp.float32)


def levels(key, extent, cuts, least, largest):
    level, own = 1.0, jax.random.fold_in(key, 6)
    for dim, blocks in cuts:
        heights = jnp.exp(jax.random.uniform(jax.random.fold_in(own, dim), (blocks,), jnp.float32, least / len(cuts), largest / len(cuts)))
        level = level * jnp.repeat(heights, extent[dim] // blocks).reshape([-1 if axis == dim else 1 for axis in range(len(extent))])
    return level


def centred(key, shape, scale, limit, pieces=(), kind=jnp.bfloat16):
    array = scale * jax.random.normal(key, shape, jnp.float32)
    if pieces:
        array = array * levels(key, shape, pieces, -0.22, 0.18)
    return jnp.clip(array, -limit, limit).astype(kind)


def setup_inputs(seed: int = 0) -> dict:
    keys = jax.random.split(jax.random.key(seed), 13)
    activations = draw_activations(jax.random.fold_in(keys[12], 71), 0)
    norm_gain = jnp.clip(1.0 + 0.18 * jax.random.normal(keys[1], (D,), jnp.float32), 0.1, 1.9)
    w_value = centred(keys[2], (D, C), D ** -0.5, 0.125, ((0, 4), (1, 4)))
    w_gate_conv = centred(keys[3], (D, C), D ** -0.5, 0.125, ((0, 4), (1, 4)))
    conv_weight = draw_conv_weight(jax.random.fold_in(keys[12], 71), 0)
    chan_gain = jnp.clip(1.0 + 0.18 * jax.random.normal(keys[5], (C,), jnp.float32), 0.1, 1.9)
    w_conv_out = centred(keys[6], (C, D), C ** -0.5, 0.125, ((0, 4), (1, 4)))
    mix_gain = jnp.clip(1.0 + 0.18 * jax.random.normal(keys[7], (D,), jnp.float32), 0.1, 1.9)
    w_gate = centred(keys[8], (D, FF), D ** -0.5, 0.125, ((0, 4), (1, 4)))
    w_up = centred(keys[9], (D, FF), D ** -0.5, 0.125, ((0, 4), (1, 4)))
    w_down = centred(keys[10], (FF, D), FF ** -0.5, 0.109375, ((0, 4), (1, 4)))
    final_gain = jnp.clip(1.0 + 0.18 * jax.random.normal(keys[11], (D,), jnp.float32), 0.1, 1.9)
    return {"activations": activations, "norm_gain": norm_gain, "w_value": w_value, "w_gate_conv": w_gate_conv, "conv_weight": conv_weight, "chan_gain": chan_gain, "w_conv_out": w_conv_out, "mix_gain": mix_gain, "w_gate": w_gate, "w_up": w_up, "w_down": w_down, "final_gain": final_gain}


EPS = 1e-06

def rms_scale(values, gain):
    return values * lax.rsqrt(lax.optimization_barrier(jnp.mean(values * values, axis=-1, keepdims=True)) + EPS) * gain

def blocked_product(left, weight):
    span = weight.shape[0] // N_TP
    total = jnp.zeros((left.shape[0], weight.shape[1]), jnp.float32)
    for block in range(N_TP):
        part = jnp.dot(left[:, block * span:(block + 1) * span], weight[block * span:(block + 1) * span], preferred_element_type=jnp.float32).astype(jnp.bfloat16)
        part = lax.optimization_barrier(part)
        total = total + part.astype(jnp.float32)
    return total

def reference(activations, norm_gain, w_value, w_gate_conv, conv_weight, chan_gain, w_conv_out, mix_gain, w_gate, w_up, w_down, final_gain):

    def one_sequence(sequence):
        residual = sequence.astype(jnp.float32)
        normed_in = rms_scale(residual, norm_gain).astype(jnp.bfloat16)
        value = jnp.dot(normed_in, w_value, preferred_element_type=jnp.float32)
        gate_conv = jnp.dot(normed_in, w_gate_conv, preferred_element_type=jnp.float32)
        glu = value * jax.nn.sigmoid(gate_conv)
        padded = jnp.pad(glu, ((K - 1, 0), (0, 0)))
        conv = jnp.zeros_like(glu)
        for tap in range(K):
            conv = conv + conv_weight[tap][None, :] * padded[tap:tap + SEQ]
        mean = lax.optimization_barrier(jnp.mean(conv, axis=-1, keepdims=True))
        centered = conv - mean
        spread = lax.optimization_barrier(jnp.mean(centered * centered, axis=-1, keepdims=True))
        act = jax.nn.silu(centered * lax.rsqrt(spread + EPS) * chan_gain).astype(jnp.bfloat16)
        first = (residual + blocked_product(act, w_conv_out)).astype(jnp.bfloat16)
        first_f = first.astype(jnp.float32)
        normed_mid = rms_scale(first_f, mix_gain).astype(jnp.bfloat16)
        gate = jnp.dot(normed_mid, w_gate, preferred_element_type=jnp.float32)
        up = jnp.dot(normed_mid, w_up, preferred_element_type=jnp.float32)
        hidden = (jax.nn.silu(gate) * up).astype(jnp.bfloat16)
        second = first_f + blocked_product(hidden, w_down)
        return rms_scale(second, final_gain).astype(jnp.bfloat16)
    return lax.map(one_sequence, activations)
```

```python
import functools

import jax
import jax.numpy as jnp
from jax import lax
from jax.experimental import pallas as pl
from jax.experimental.pallas import tpu as pltpu
from jax.sharding import PartitionSpec as P

EPS = 1e-06
MESH = pl.DeviceIdType.MESH
F32 = jnp.float32
BF16 = jnp.bfloat16


def remote(src, dst, send, recv, target):
    return pltpu.make_async_remote_copy(
        src_ref=src, dst_ref=dst, send_sem=send, recv_sem=recv, device_id=target, device_id_type=MESH
    )


def chunk_of(extent, want):
    return want if extent % want == 0 else extent


def kernel(
    R, F, T, split, length,
    x_ref, ng_ref, cw_ref, cg_ref, mg_ref, fg_ref,
    wv_ref, wg_ref, wo_ref, wga_ref, wup_ref, wd_ref,
    out_ref,
    bv, bg, bo, bga, bup, bd,
    xg, rows, glu, conv, act, part1, part2, got1, got2, firsts, hid, st1, st2, sg1, sg2,
    own_sem, zs, zr, ys, yr, ts, tr,
):
    f = lax.axis_index("fs")
    me = lax.axis_index("tp")
    rep = lax.axis_index("rep")
    count, dt = x_ref.shape
    width = dt * T
    local = [wv_ref, wg_ref, wo_ref, wga_ref, wup_ref, wd_ref]
    bufs = [bv, bg, bo, bga, bup, bd]

    barrier = pltpu.get_barrier_semaphore()
    greeted = 0
    for target in (lax.rem(f + 1, F), lax.rem(f + F - 1, F)):
        pl.semaphore_signal(barrier, inc=1, device_id={"fs": target}, device_id_type=MESH)
        greeted += 1
    if split == 2:
        pl.semaphore_signal(barrier, inc=1, device_id={"rep": 1 - rep}, device_id_type=MESH)
        greeted += 1
    for d in range(1, T):
        pl.semaphore_signal(barrier, inc=1, device_id={"tp": lax.rem(me + d, T)}, device_id_type=MESH)
        greeted += 1
    own = [
        pltpu.make_async_copy(local[w], bufs[w].at[f], own_sem.at[w]) for w in range(6)
    ]
    for copy in own:
        copy.start()
    pl.semaphore_wait(barrier, greeted)

    def half(w):
        n = local[w].shape[0] // split
        return pl.ds(pl.multiple_of((rep if split == 2 else 0) * n, n), n)

    def other(w):
        n = local[w].shape[0] // split
        return pl.ds(pl.multiple_of((1 - rep) * n, n), n)

    def hop(w, side, s):
        shard = f - s if side == 0 else f + s
        target = f + 1 if side == 0 else f - 1
        src = local[w].at[half(w)] if s == 0 else bufs[w].at[shard, half(w)]
        return remote(src, bufs[w].at[shard, half(w)], zs.at[side, w, s], zr.at[side, w, s + 1], {"fs": target})

    def arrival(w, side, s):
        shard = f - s if side == 0 else f + s
        ref = bufs[w].at[shard, half(w)]
        return remote(ref, ref, zs.at[side, w, s], zr.at[side, w, s], {"fs": f})

    def across(w, side, s):
        shard = f - s if side == 0 else f + s
        ref = bufs[w].at[shard, half(w)]
        return remote(ref, ref, ys.at[side, w, s], yr.at[side, w, s], {"rep": 1 - rep})

    def across_in(w, side, s):
        shard = f - s if side == 0 else f + s
        ref = bufs[w].at[shard, other(w)]
        return remote(ref, ref, ys.at[side, w, s], yr.at[side, w, s], {"rep": 1 - rep})

    def has(side, s):
        return f >= s if side == 0 else f + s <= F - 1

    def sends(side, s):
        ahead = f < F - 1 if side == 0 else f > 0
        return jnp.logical_and(has(side, s), ahead)

    def launch(w):
        for side in (0, 1):
            @pl.when(sends(side, 0))
            def _():
                hop(w, side, 0).start()

    def relay(group):
        for s in range(1, F):
            for w in group:
                for side in (0, 1):
                    @pl.when(has(side, s))
                    def _():
                        arrival(w, side, s).wait_recv()
                        if s < F - 1:
                            @pl.when(sends(side, s))
                            def _():
                                hop(w, side, s).start()
                        if split == 2:
                            across(w, side, s).start()

    def settle(group):
        for w in group:
            own[w].wait()
        if split == 2:
            for s in range(1, F):
                for w in group:
                    for side in (0, 1):
                        @pl.when(has(side, s))
                        def _():
                            across_in(w, side, s).wait_recv()

    def tp_send(k, src, dst_at, d):
        return remote(src, dst_at, ts.at[k, d], tr.at[k, d], {"tp": lax.rem(me + d, T)})

    for w in (0, 1):
        launch(w)
    for d in range(1, T):
        tp_send(0, x_ref, xg.at[me], d).start()
    launch(2)
    xg[me] = x_ref[...]
    for d in range(1, T):
        peer = lax.rem(me + T - d, T)
        tp_send(0, x_ref, xg.at[peer], d).wait_recv()

    block = chunk_of(count, 16)

    def norm_rows(src, gain):
        def step(i, _):
            r = pl.ds(pl.multiple_of(i * block, block), block)
            vals = [src[t, r, :].astype(F32) for t in range(T)]
            ss = sum(jnp.sum(v * v, axis=1, keepdims=True) for v in vals)
            scale = lax.rsqrt(ss / width + EPS)
            for t in range(T):
                rows[r, t * dt:(t + 1) * dt] = (
                    vals[t] * scale * gain[t:t + 1, :]
                ).astype(BF16)
            return 0
        lax.fori_loop(0, count // block, step, 0)

    norm_rows(xg, ng_ref)
    relay((0, 1))
    launch(3)
    launch(4)
    settle((0, 1))

    chan = bv.shape[2]
    batch = count // length
    taps = cw_ref.shape[0]
    pad = 8 * ((taps - 1 + 7) // 8)
    lead = pad - (taps - 1)

    def columns(buf, c, n):
        block_w = buf[:, :, pl.ds(pl.multiple_of(c * n, n), n)]
        return block_w.reshape(block_w.shape[0] * block_w.shape[1], n)

    nc = chunk_of(chan, 256)

    def glu_step(c, _):
        value = jnp.dot(rows[...], columns(bv, c, nc), preferred_element_type=F32)
        gate = jnp.dot(rows[...], columns(bg, c, nc), preferred_element_type=F32)
        res = value * jax.nn.sigmoid(gate)
        for b in range(batch):
            glu[b, pl.ds(pad, length), pl.ds(pl.multiple_of(c * nc, nc), nc)] = (
                res[b * length:(b + 1) * length]
            )
        return 0

    for b in range(batch):
        glu[b, 0:pad, :] = jnp.zeros((pad, chan), F32)
        glu[b, pad + length:, :] = jnp.zeros((8, chan), F32)
    lax.fori_loop(0, chan // nc, glu_step, 0)

    lanes = chunk_of(chan, 128)
    span = chunk_of(length, 64)
    strips = chan // lanes

    def conv_step(i, _):
        q = lax.rem(i, strips)
        p = i // strips
        cols = pl.ds(pl.multiple_of(q * lanes, lanes), lanes)
        weights = cw_ref[:, cols]
        for b in range(batch):
            total = jnp.zeros((span, lanes), F32)
            for shift in range(8):
                acc = None
                for tap in range(taps):
                    if (lead + tap) % 8 != shift:
                        continue
                    base = lead + tap - shift
                    term = weights[tap:tap + 1, :] * glu[
                        b, pl.ds(pl.multiple_of(p * span + base, 8), span + 8), cols
                    ]
                    acc = term if acc is None else acc + term
                if acc is not None:
                    total = total + acc[shift:shift + span]
            conv[pl.ds(pl.multiple_of(b * length + p * span, span), span), cols] = total
        return 0

    lax.fori_loop(0, strips * (length // span), conv_step, 0)

    lane = lax.broadcasted_iota(jnp.int32, (count, 128), 1)

    def across_lanes(a, b):
        table = jnp.where(lane == 0, a, jnp.where(lane == 1, b, 0.0))
        return jnp.transpose(table)[0:8, :]

    def down_rows(top):
        full = jnp.concatenate([top, jnp.zeros((120, count), F32)], axis=0)
        return jnp.transpose(full)

    values = conv[...]
    local_sum = jnp.sum(values, axis=1, keepdims=True)
    dev = values - local_sum / chan
    st1[...] = across_lanes(local_sum, jnp.sum(dev * dev, axis=1, keepdims=True))
    sg1[me] = st1[...]
    for d in range(1, T):
        tp_send(1, st1, sg1.at[me], d).start()
    relay((2,))
    launch(5)
    for d in range(1, T):
        peer = lax.rem(me + T - d, T)
        tp_send(1, st1, sg1.at[peer], d).wait_recv()
    sums = [sg1[t] for t in range(T)]
    mean = sum(s[0:1, :] for s in sums) / (chan * T)
    spread = sum(
        s[1:2, :] + chan * (s[0:1, :] / chan - mean) * (s[0:1, :] / chan - mean) for s in sums
    ) / (chan * T)
    inv = lax.rsqrt(spread + EPS)
    line = lax.broadcasted_iota(jnp.int32, (8, count), 0)
    table = down_rows(jnp.where(line == 0, mean, jnp.where(line == 1, inv, 0.0)))
    normed = (conv[...] - table[:, 0:1]) * table[:, 1:2] * cg_ref[...]
    act[...] = (normed * jax.nn.sigmoid(normed)).astype(BF16)

    settle((2,))

    def project(src, buf, part):
        dsh = buf.shape[2]
        for j in range(F):
            t, off = (j * dsh) // dt, (j * dsh) % dt
            prod = jnp.dot(src[...], buf[j], preferred_element_type=F32)
            part[t, :, off:off + dsh] = prod.astype(BF16)

    def scatter(k, part, got):
        for d in range(1, T):
            tp_send(k, part.at[lax.rem(me + d, T)], got.at[d - 1], d).start()

    def gathered(k, part, got):
        total = part[me].astype(F32)
        for d in range(1, T):
            tp_send(k, part.at[me], got.at[d - 1], d).wait_recv()
            total = total + got[d - 1].astype(F32)
        return total

    project(act, bo, part1)
    scatter(2, part1, got1)
    first = (x_ref[...].astype(F32) + gathered(2, part1, got1)).astype(BF16)
    firsts[me] = first
    for d in range(1, T):
        tp_send(3, firsts.at[me], firsts.at[me], d).start()
    relay((3, 4))
    for d in range(1, T):
        peer = lax.rem(me + T - d, T)
        tp_send(3, firsts.at[peer], firsts.at[peer], d).wait_recv()
    norm_rows(firsts, mg_ref)
    settle((3, 4))

    ff = bga.shape[2]
    nf = chunk_of(ff, 256)

    def ff_step(c, _):
        gate = jnp.dot(rows[...], columns(bga, c, nf), preferred_element_type=F32)
        up = jnp.dot(rows[...], columns(bup, c, nf), preferred_element_type=F32)
        hid[:, pl.ds(pl.multiple_of(c * nf, nf), nf)] = (
            gate * jax.nn.sigmoid(gate) * up
        ).astype(BF16)
        return 0

    lax.fori_loop(0, ff // nf, ff_step, 0)
    relay((5,))
    settle((5,))
    project(hid, bd, part2)
    scatter(4, part2, got2)
    second = firsts[me].astype(F32) + gathered(4, part2, got2)
    total = jnp.sum(second * second, axis=1, keepdims=True)
    conv[:, 0:dt] = second
    st2[...] = across_lanes(total, total)
    sg2[me] = st2[...]
    for d in range(1, T):
        tp_send(5, st2, sg2.at[me], d).start()
    for d in range(1, T):
        peer = lax.rem(me + T - d, T)
        tp_send(5, st2, sg2.at[peer], d).wait_recv()
    full = sum(sg2[t] for t in range(T))
    table = down_rows(full)
    scale = lax.rsqrt(table[:, 0:1] / width + EPS)
    out_ref[...] = (conv[:, 0:dt] * scale * fg_ref[...]).astype(BF16)

    for w in range(6):
        for side in (0, 1):
            for s in range(F):
                if s < F - 1:
                    @pl.when(sends(side, s))
                    def _():
                        hop(w, side, s).wait_send()
                if s >= 1 and split == 2:
                    @pl.when(has(side, s))
                    def _():
                        across(w, side, s).wait_send()
    for d in range(1, T):
        peer = lax.rem(me + d, T)
        tp_send(0, x_ref, xg.at[me], d).wait_send()
        tp_send(1, st1, sg1.at[me], d).wait_send()
        tp_send(2, part1.at[peer], got1.at[d - 1], d).wait_send()
        tp_send(3, firsts.at[me], firsts.at[me], d).wait_send()
        tp_send(4, part2.at[peer], got2.at[d - 1], d).wait_send()
        tp_send(5, st2, sg2.at[me], d).wait_send()


def body(
    activations, norm_gain, w_value, w_gate_conv, conv_weight, chan_gain,
    w_conv_out, mix_gain, w_gate, w_up, w_down, final_gain,
):
    batch, length, dt = activations.shape
    count = batch * length
    R, F, T = lax.axis_size("rep"), lax.axis_size("fs"), lax.axis_size("tp")
    weights = (w_value, w_gate_conv, w_conv_out, w_gate, w_up, w_down)
    split = 2 if R == 2 and all(w.shape[0] % 32 == 0 for w in weights) else 1
    width = dt * T
    chan, ff = w_value.shape[1], w_gate.shape[1]
    taps = conv_weight.shape[0]
    pad = 8 * ((taps - 1 + 7) // 8)
    vmem, hbm = pl.BlockSpec(memory_space=pltpu.VMEM), pl.BlockSpec(memory_space=pl.ANY)
    ysh = (2, 6, F) if split == 2 else (1,)
    dma = pltpu.SemaphoreType.DMA
    out = pl.pallas_call(
        functools.partial(kernel, R, F, T, split, length),
        out_shape=jax.ShapeDtypeStruct((count, dt), BF16),
        in_specs=[vmem] * 6 + [hbm] * 6,
        out_specs=vmem,
        scratch_shapes=[pltpu.VMEM((F,) + w.shape, BF16) for w in weights] + [
            pltpu.VMEM((T, count, dt), BF16),
            pltpu.VMEM((count, width), BF16),
            pltpu.VMEM((batch, pad + length + 8, chan), F32),
            pltpu.VMEM((count, max(chan, dt)), F32),
            pltpu.VMEM((count, chan), BF16),
            pltpu.VMEM((T, count, dt), BF16),
            pltpu.VMEM((T, count, dt), BF16),
            pltpu.VMEM((T - 1, count, dt), BF16),
            pltpu.VMEM((T - 1, count, dt), BF16),
            pltpu.VMEM((T, count, dt), BF16),
            pltpu.VMEM((count, ff), BF16),
            pltpu.VMEM((8, count), F32),
            pltpu.VMEM((8, count), F32),
            pltpu.VMEM((T, 8, count), F32),
            pltpu.VMEM((T, 8, count), F32),
            dma((6,)),
            dma((2, 6, F)),
            dma((2, 6, F)),
            dma(ysh),
            dma(ysh),
            dma((6, T)),
            dma((6, T)),
        ],
        compiler_params=pltpu.CompilerParams(
            collective_id=0, has_side_effects=True, vmem_limit_bytes=60 * 1024 * 1024
        ),
        name="block",
    )(
        activations.reshape(count, dt),
        norm_gain.reshape(T, dt),
        conv_weight,
        chan_gain.reshape(1, chan),
        mix_gain.reshape(T, dt),
        final_gain.reshape(1, dt),
        *weights,
    )
    return out.reshape(batch, length, dt)


def solution(mesh):
    in_specs = (
        P(("rep", "fs"), None, "tp"),
        P(),
        P("fs", "tp"),
        P("fs", "tp"),
        P(None, "tp"),
        P("tp"),
        P("tp", "fs"),
        P(),
        P("fs", "tp"),
        P("fs", "tp"),
        P("tp", "fs"),
        P("tp"),
    )
    out_specs = P(("rep", "fs"), None, "tp")
    return jax.shard_map(body, mesh=mesh, in_specs=in_specs, out_specs=out_specs, check_vma=False)
```

```python
import functools

import jax
import jax.numpy as jnp
from jax import lax
from jax.experimental import pallas as pl
from jax.experimental.pallas import tpu as pltpu
from jax.sharding import PartitionSpec as P

EPS = 1e-06
MESH = pl.DeviceIdType.MESH
F32 = jnp.float32
BF16 = jnp.bfloat16


def remote(src, dst, send, recv, target):
    return pltpu.make_async_remote_copy(
        src_ref=src, dst_ref=dst, send_sem=send, recv_sem=recv, device_id=target, device_id_type=MESH
    )


def chunk_of(extent, want):
    return want if extent % want == 0 else extent


def kernel(
    R, F, T, split, length,
    x_ref, ng_ref, cw_ref, cg_ref, mg_ref, fg_ref,
    wv_ref, wg_ref, wo_ref, wga_ref, wup_ref, wd_ref,
    out_ref,
    bv, bg, bo, bga, bup, bd,
    xg, rows, glu, conv, act, part1, part2, got1, got2, firsts, hid, st1, st2, sg1, sg2,
    own_sem, zs, zr, ys, yr, ts, tr,
):
    f = lax.axis_index("fs")
    me = lax.axis_index("tp")
    rep = lax.axis_index("rep")
    count, dt = x_ref.shape
    width = dt * T
    local = [wv_ref, wg_ref, wo_ref, wga_ref, wup_ref, wd_ref]
    bufs = [bv, bg, bo, bga, bup, bd]

    barrier = pltpu.get_barrier_semaphore()
    greeted = 0
    for target in (lax.rem(f + 1, F), lax.rem(f + F - 1, F)):
        pl.semaphore_signal(barrier, inc=1, device_id={"fs": target}, device_id_type=MESH)
        greeted += 1
    if split == 2:
        pl.semaphore_signal(barrier, inc=1, device_id={"rep": 1 - rep}, device_id_type=MESH)
        greeted += 1
    for d in range(1, T):
        pl.semaphore_signal(barrier, inc=1, device_id={"tp": lax.rem(me + d, T)}, device_id_type=MESH)
        greeted += 1
    own = [
        pltpu.make_async_copy(local[w], bufs[w].at[f], own_sem.at[w]) for w in range(6)
    ]
    for copy in own:
        copy.start()
    pl.semaphore_wait(barrier, greeted)

    def half(w):
        n = local[w].shape[0] // split
        return pl.ds(pl.multiple_of((rep if split == 2 else 0) * n, n), n)

    def other(w):
        n = local[w].shape[0] // split
        return pl.ds(pl.multiple_of((1 - rep) * n, n), n)

    def hop(w, side, s):
        shard = f - s if side == 0 else f + s
        target = f + 1 if side == 0 else f - 1
        src = local[w].at[half(w)] if s == 0 else bufs[w].at[shard, half(w)]
        return remote(src, bufs[w].at[shard, half(w)], zs.at[side, w, s], zr.at[side, w, s + 1], {"fs": target})

    def arrival(w, side, s):
        shard = f - s if side == 0 else f + s
        ref = bufs[w].at[shard, half(w)]
        return remote(ref, ref, zs.at[side, w, s], zr.at[side, w, s], {"fs": f})

    def across(w, side, s):
        shard = f - s if side == 0 else f + s
        ref = bufs[w].at[shard, half(w)]
        return remote(ref, ref, ys.at[side, w, s], yr.at[side, w, s], {"rep": 1 - rep})

    def across_in(w, side, s):
        shard = f - s if side == 0 else f + s
        ref = bufs[w].at[shard, other(w)]
        return remote(ref, ref, ys.at[side, w, s], yr.at[side, w, s], {"rep": 1 - rep})

    def has(side, s):
        return f >= s if side == 0 else f + s <= F - 1

    def sends(side, s):
        ahead = f < F - 1 if side == 0 else f > 0
        return jnp.logical_and(has(side, s), ahead)

    def launch(w):
        for side in (0, 1):
            @pl.when(sends(side, 0))
            def _():
                hop(w, side, 0).start()

    def relay(group, stages=range(1, F)):
        for s in stages:
            for w in group:
                for side in (0, 1):
                    @pl.when(has(side, s))
                    def _():
                        arrival(w, side, s).wait_recv()
                        if s < F - 1:
                            @pl.when(sends(side, s))
                            def _():
                                hop(w, side, s).start()
                        if split == 2:
                            across(w, side, s).start()

    def settle(group):
        for w in group:
            own[w].wait()
        if split == 2:
            for s in range(1, F):
                for w in group:
                    for side in (0, 1):
                        @pl.when(has(side, s))
                        def _():
                            across_in(w, side, s).wait_recv()

    def tp_send(k, src, dst_at, d):
        return remote(src, dst_at, ts.at[k, d], tr.at[k, d], {"tp": lax.rem(me + d, T)})

    for w in (0, 1):
        launch(w)
    for d in range(1, T):
        tp_send(0, x_ref, xg.at[me], d).start()
    launch(2)
    xg[me] = x_ref[...]
    for d in range(1, T):
        peer = lax.rem(me + T - d, T)
        tp_send(0, x_ref, xg.at[peer], d).wait_recv()

    block = chunk_of(count, 16)

    def norm_rows(src, gain):
        def step(i, _):
            r = pl.ds(pl.multiple_of(i * block, block), block)
            vals = [src[t, r, :].astype(F32) for t in range(T)]
            ss = sum(jnp.sum(v * v, axis=1, keepdims=True) for v in vals)
            scale = lax.rsqrt(ss / width + EPS)
            for t in range(T):
                rows[r, t * dt:(t + 1) * dt] = (
                    vals[t] * scale * gain[t:t + 1, :]
                ).astype(BF16)
            return 0
        lax.fori_loop(0, count // block, step, 0)

    norm_rows(xg, ng_ref)
    relay((0, 1, 2))
    for w in (3, 4, 5):
        launch(w)
    settle((0, 1))

    chan = bv.shape[2]
    batch = count // length
    taps = cw_ref.shape[0]
    pad = 8 * ((taps - 1 + 7) // 8)
    lead = pad - (taps - 1)

    def columns(buf, c, n):
        block_w = buf[:, :, pl.ds(pl.multiple_of(c * n, n), n)]
        return block_w.reshape(block_w.shape[0] * block_w.shape[1], n)

    nc = chunk_of(chan, 256)

    def glu_step(c, _):
        value = jnp.dot(rows[...], columns(bv, c, nc), preferred_element_type=F32)
        gate = jnp.dot(rows[...], columns(bg, c, nc), preferred_element_type=F32)
        res = value * jax.nn.sigmoid(gate)
        for b in range(batch):
            glu[b, pl.ds(pad, length), pl.ds(pl.multiple_of(c * nc, nc), nc)] = (
                res[b * length:(b + 1) * length]
            )
        return 0

    for b in range(batch):
        glu[b, 0:pad, :] = jnp.zeros((pad, chan), F32)
        glu[b, pad + length:, :] = jnp.zeros((8, chan), F32)
    lax.fori_loop(0, chan // nc, glu_step, 0)
    relay((3,), (1,))

    lanes = chunk_of(chan, 128)
    span = chunk_of(length, 64)
    strips = chan // lanes

    def conv_step(i, _):
        q = lax.rem(i, strips)
        p = i // strips
        cols = pl.ds(pl.multiple_of(q * lanes, lanes), lanes)
        weights = cw_ref[:, cols]
        for b in range(batch):
            total = jnp.zeros((span, lanes), F32)
            for shift in range(8):
                acc = None
                for tap in range(taps):
                    if (lead + tap) % 8 != shift:
                        continue
                    base = lead + tap - shift
                    term = weights[tap:tap + 1, :] * glu[
                        b, pl.ds(pl.multiple_of(p * span + base, 8), span + 8), cols
                    ]
                    acc = term if acc is None else acc + term
                if acc is not None:
                    total = total + acc[shift:shift + span]
            conv[pl.ds(pl.multiple_of(b * length + p * span, span), span), cols] = total
        return 0

    lax.fori_loop(0, strips * (length // span), conv_step, 0)

    lane = lax.broadcasted_iota(jnp.int32, (count, 128), 1)

    def across_lanes(a, b):
        table = jnp.where(lane == 0, a, jnp.where(lane == 1, b, 0.0))
        return jnp.transpose(table)[0:8, :]

    def down_rows(top):
        full = jnp.concatenate([top, jnp.zeros((120, count), F32)], axis=0)
        return jnp.transpose(full)

    values = conv[...]
    local_sum = jnp.sum(values, axis=1, keepdims=True)
    dev = values - local_sum / chan
    st1[...] = across_lanes(local_sum, jnp.sum(dev * dev, axis=1, keepdims=True))
    sg1[me] = st1[...]
    for d in range(1, T):
        tp_send(1, st1, sg1.at[me], d).start()
    relay((4,), (1,))
    for d in range(1, T):
        peer = lax.rem(me + T - d, T)
        tp_send(1, st1, sg1.at[peer], d).wait_recv()
    sums = [sg1[t] for t in range(T)]
    mean = sum(s[0:1, :] for s in sums) / (chan * T)
    spread = sum(
        s[1:2, :] + chan * (s[0:1, :] / chan - mean) * (s[0:1, :] / chan - mean) for s in sums
    ) / (chan * T)
    inv = lax.rsqrt(spread + EPS)
    line = lax.broadcasted_iota(jnp.int32, (8, count), 0)
    table = down_rows(jnp.where(line == 0, mean, jnp.where(line == 1, inv, 0.0)))
    normed = (conv[...] - table[:, 0:1]) * table[:, 1:2] * cg_ref[...]
    act[...] = (normed * jax.nn.sigmoid(normed)).astype(BF16)

    settle((2,))

    def project(src, buf, part):
        dsh = buf.shape[2]
        for j in range(F):
            t, off = (j * dsh) // dt, (j * dsh) % dt
            prod = jnp.dot(src[...], buf[j], preferred_element_type=F32)
            part[t, :, off:off + dsh] = prod.astype(BF16)

    def scatter(k, part, got):
        for d in range(1, T):
            tp_send(k, part.at[lax.rem(me + d, T)], got.at[d - 1], d).start()

    def gathered(k, part, got):
        total = part[me].astype(F32)
        for d in range(1, T):
            tp_send(k, part.at[me], got.at[d - 1], d).wait_recv()
            total = total + got[d - 1].astype(F32)
        return total

    def piece(t):
        return remote(part2.at[t], got2.at[me], ts.at[4, t], tr.at[4, me], {"tp": t})

    def piece_in(t):
        return remote(part2.at[t], got2.at[t], ts.at[4, t], tr.at[4, t], {"tp": t})

    project(act, bo, part1)
    scatter(2, part1, got1)
    relay((5,), (1,))
    first = (x_ref[...].astype(F32) + gathered(2, part1, got1)).astype(BF16)
    firsts[me] = first
    for d in range(1, T):
        tp_send(3, firsts.at[me], firsts.at[me], d).start()
    relay((3,), (2,))
    for d in range(1, T):
        peer = lax.rem(me + T - d, T)
        tp_send(3, firsts.at[peer], firsts.at[peer], d).wait_recv()
    relay((4,), (2,))
    norm_rows(firsts, mg_ref)
    relay((5,), (2,))
    relay((3, 4), range(3, F))
    settle((3, 4))

    ff = bga.shape[2]
    nf = chunk_of(ff, 256)

    def ff_step(c, _):
        gate = jnp.dot(rows[...], columns(bga, c, nf), preferred_element_type=F32)
        up = jnp.dot(rows[...], columns(bup, c, nf), preferred_element_type=F32)
        hid[:, pl.ds(pl.multiple_of(c * nf, nf), nf)] = (
            gate * jax.nn.sigmoid(gate) * up
        ).astype(BF16)
        return 0

    lax.fori_loop(0, ff // nf, ff_step, 0)
    if F == T and bd.shape[2] == dt:
        def down(shard):
            prod = jnp.dot(hid[...], bd[shard], preferred_element_type=F32)
            part2[shard] = prod.astype(BF16)

            @pl.when(shard != me)
            def _():
                piece(shard).start()

        own[5].wait()
        down(f)
        for s in range(1, F):
            if s >= 3:
                relay((5,), (s,))
            for side in (0, 1):
                @pl.when(has(side, s))
                def _():
                    if split == 2:
                        across_in(5, side, s).wait_recv()
                    down(f - s if side == 0 else f + s)
    else:
        relay((5,), range(3, F))
        settle((5,))
        project(hid, bd, part2)
        for d in range(1, T):
            piece(lax.rem(me + d, T)).start()
    second = firsts[me].astype(F32) + part2[me].astype(F32)
    for d in range(1, T):
        peer = lax.rem(me + d, T)
        piece_in(peer).wait_recv()
        second = second + got2[peer].astype(F32)
    total = jnp.sum(second * second, axis=1, keepdims=True)
    conv[:, 0:dt] = second
    st2[...] = across_lanes(total, total)
    sg2[me] = st2[...]
    for d in range(1, T):
        tp_send(5, st2, sg2.at[me], d).start()
    for d in range(1, T):
        peer = lax.rem(me + T - d, T)
        tp_send(5, st2, sg2.at[peer], d).wait_recv()
    full = sum(sg2[t] for t in range(T))
    table = down_rows(full)
    scale = lax.rsqrt(table[:, 0:1] / width + EPS)
    out_ref[...] = (conv[:, 0:dt] * scale * fg_ref[...]).astype(BF16)

    for w in range(6):
        for side in (0, 1):
            for s in range(F):
                if s < F - 1:
                    @pl.when(sends(side, s))
                    def _():
                        hop(w, side, s).wait_send()
                if s >= 1 and split == 2:
                    @pl.when(has(side, s))
                    def _():
                        across(w, side, s).wait_send()
    for d in range(1, T):
        peer = lax.rem(me + d, T)
        tp_send(0, x_ref, xg.at[me], d).wait_send()
        tp_send(1, st1, sg1.at[me], d).wait_send()
        tp_send(2, part1.at[peer], got1.at[d - 1], d).wait_send()
        tp_send(3, firsts.at[me], firsts.at[me], d).wait_send()
        piece(peer).wait_send()
        tp_send(5, st2, sg2.at[me], d).wait_send()


def body(
    activations, norm_gain, w_value, w_gate_conv, conv_weight, chan_gain,
    w_conv_out, mix_gain, w_gate, w_up, w_down, final_gain,
):
    batch, length, dt = activations.shape
    count = batch * length
    R, F, T = lax.axis_size("rep"), lax.axis_size("fs"), lax.axis_size("tp")
    weights = (w_value, w_gate_conv, w_conv_out, w_gate, w_up, w_down)
    split = 2 if R == 2 and all(w.shape[0] % 32 == 0 for w in weights) else 1
    width = dt * T
    chan, ff = w_value.shape[1], w_gate.shape[1]
    taps = conv_weight.shape[0]
    pad = 8 * ((taps - 1 + 7) // 8)
    vmem, hbm = pl.BlockSpec(memory_space=pltpu.VMEM), pl.BlockSpec(memory_space=pl.ANY)
    ysh = (2, 6, F) if split == 2 else (1,)
    dma = pltpu.SemaphoreType.DMA
    out = pl.pallas_call(
        functools.partial(kernel, R, F, T, split, length),
        out_shape=jax.ShapeDtypeStruct((count, dt), BF16),
        in_specs=[vmem] * 6 + [hbm] * 6,
        out_specs=vmem,
        scratch_shapes=[pltpu.VMEM((F,) + w.shape, BF16) for w in weights] + [
            pltpu.VMEM((T, count, dt), BF16),
            pltpu.VMEM((count, width), BF16),
            pltpu.VMEM((batch, pad + length + 8, chan), F32),
            pltpu.VMEM((count, max(chan, dt)), F32),
            pltpu.VMEM((count, chan), BF16),
            pltpu.VMEM((T, count, dt), BF16),
            pltpu.VMEM((T, count, dt), BF16),
            pltpu.VMEM((T - 1, count, dt), BF16),
            pltpu.VMEM((T, count, dt), BF16),
            pltpu.VMEM((T, count, dt), BF16),
            pltpu.VMEM((count, ff), BF16),
            pltpu.VMEM((8, count), F32),
            pltpu.VMEM((8, count), F32),
            pltpu.VMEM((T, 8, count), F32),
            pltpu.VMEM((T, 8, count), F32),
            dma((6,)),
            dma((2, 6, F)),
            dma((2, 6, F)),
            dma(ysh),
            dma(ysh),
            dma((6, T)),
            dma((6, T)),
        ],
        compiler_params=pltpu.CompilerParams(
            collective_id=0, has_side_effects=True, vmem_limit_bytes=60 * 1024 * 1024
        ),
        name="block",
    )(
        activations.reshape(count, dt),
        norm_gain.reshape(T, dt),
        conv_weight,
        chan_gain.reshape(1, chan),
        mix_gain.reshape(T, dt),
        final_gain.reshape(1, dt),
        *weights,
    )
    return out.reshape(batch, length, dt)


def solution(mesh):
    in_specs = (
        P(("rep", "fs"), None, "tp"),
        P(),
        P("fs", "tp"),
        P("fs", "tp"),
        P(None, "tp"),
        P("tp"),
        P("tp", "fs"),
        P(),
        P("fs", "tp"),
        P("fs", "tp"),
        P("tp", "fs"),
        P("tp"),
    )
    out_specs = P(("rep", "fs"), None, "tp")
    return jax.shard_map(body, mesh=mesh, in_specs=in_specs, out_specs=out_specs, check_vma=False)
```
